32 devices in a mesh: ep: 16 (over z, y, x), tp: 2 (over core).
Axes of the slice: x: 2, y: 2, z: 4, core: 2. Of those that a mesh axis runs over, the one named last changes fastest.
Arguments:
- tokens: bfloat16 [512, 2048], P('ep'), may hold values from -6 to 6
- mix_gain: float32 [2048], replicated, may hold values from 0.1 to 1.9
- w_query: bfloat16 [2048, 512], P('ep', 'tp'), may hold values from -0.125 to 0.125
- w_key: bfloat16 [2048, 512], P('ep', 'tp'), may hold values from -0.125 to 0.125
- w_value: bfloat16 [2048, 512], P('ep', 'tp'), may hold values from -0.125 to 0.125
- w_outgate: bfloat16 [2048, 512], P('ep', 'tp'), may hold values from -0.125 to 0.125
- w_igate: bfloat16 [2048, 8], P('ep', 'tp'), may hold values from -0.125 to 0.125
- w_fgate: bfloat16 [2048, 8], P('ep', 'tp'), may hold values from -0.125 to 0.125
- igate_bias: float32 [8], P('tp'), may hold values from -2 to 1
- fgate_bias: float32 [8], P('tp'), may hold values from 0 to 4
- head_gain: float32 [512], P('tp'), may hold values from 0.1 to 1.9
- w_out: bfloat16 [512, 2048], P('tp', 'ep'), may hold values from -0.25 to 0.25
- state_matrix: float32 [512, 8, 64, 64], P('ep', 'tp'), may hold values from -2.4 to 2.4
- state_norm: float32 [512, 8, 64], P('ep', 'tp'), may hold values from -2.4 to 2.4
- state_max: float32 [512, 8], P('ep', 'tp'), may hold values from -4 to 4
- ffn_gain: float32 [2048], replicated, may hold values from 0.1 to 1.9
- w_expert_gate: bfloat16 [16, 2048, 1408], P('ep', None, 'tp'), may hold values from -0.125 to 0.125
- w_expert_up: bfloat16 [16, 2048, 1408], P('ep', None, 'tp'), may hold values from -0.125 to 0.125
- w_expert_down: bfloat16 [16, 1408, 2048], P('ep', 'tp'), may hold values from -0.15625 to 0.15625
- routes: int32 [512, 3], P('ep'), may hold values from 0 to 15, all different within a row; in each aligned block of 32 rows (0 to 31, 32 to 63, ...) at most 12 rows name the same one
- route_weights: float32 [512, 3], P('ep'), may hold values from 0.2 to 1
Outputs:
- mixed: bfloat16 [512, 2048], P('ep')
- new_matrix: float32 [512, 8, 64, 64], P('ep', 'tp')
- new_norm: float32 [512, 8, 64], P('ep', 'tp')
- new_max: float32 [512, 8], P('ep', 'tp')
The draws below stay inside these ranges and needn't reach their ends.
Inputs may be any that keep to these rules, and one draw needn't show every extreme that they name: `routes`: each row names 3 different experts. Among the rows of one device, no expert is named by more than 12 rows, a bound that some block reaches.
All inputs are finite; a program needn't handle non-finite values.
Results may differ from the reference program's by a relative error of at most 0.017.
Values may be sent and summed in bfloat16 or wider, within the bound.
No kernel may reach another device: no remote copies, remote signals or barrier semaphores. Data moves between devices by JAX's collectives and lax.ppermute only.
A program may use at most 128 MiB of HBM per device.

```python
import math
import jax
import jax.numpy as jnp
import numpy as np
from jax import lax

D = 2048
HEADS = 8
HEAD_SIZE = 64
HW = 512
D_EXP = 1408
TOPK = 3
EXPERTS = 16
SEQ_DEV = 32
B = 512
CAP = 12
N_EP = 16
N_TP = 2


def steps_of(stream_key, shape, split, low, high):
    level = 1.0
    for position, shards_of in split:
        draws = jax.random.uniform(jax.random.fold_in(jax.random.fold_in(stream_key, 6), position), (shards_of,), jnp.float32, low / len(split), high / len(split))
        level = level * jnp.repeat(jnp.exp(draws), shape[position] // shards_of).reshape((-1,) + (1,) * (len(shape) - 1 - position))
    return level


def routed_block(stream_key, own, number, rows, amount, top, reach, lean):
    order = jax.random.permutation(stream_key, amount)
    packed, usual = load_shares(amount, rows * top, reach, lean, True), load_shares(amount, rows * top, reach, lean, False)
    places = jnp.arange(amount)

    def named(tallies, offset_by):
        used = int((tallies > 0).sum())
        fixed = max(1, used // 4)
        shifted = fixed + (places - fixed + offset_by * (used - fixed)) % max(1, amount - fixed)
        return jnp.zeros((amount,), jnp.int32).at[order[jnp.where(places < fixed, places, shifted)]].set(jnp.asarray(tallies, jnp.int32))

    tallies = jnp.where(number % 4 == 0, named(packed, number // 4), named(usual, number - number // 4 - 1))
    mixed = jax.random.permutation(jax.random.fold_in(own, 3), amount)
    source_of, sink = mixed[0:amount // 2 * 2:2], mixed[1:amount // 2 * 2:2]
    room = jnp.minimum(tallies[source_of] - 1, reach - tallies[sink]) // 2
    room = jnp.where((source_of == order[0]) | (sink == order[0]) | (tallies[sink] == 0), 0, jnp.maximum(room, 0))
    shifted = jax.random.randint(jax.random.fold_in(own, 4), (amount // 2,), 0, 1 << 20) % (room + 1)
    tallies = tallies.at[source_of].add(-shifted).at[sink].add(shifted)
    labels = jnp.searchsorted(jnp.cumsum(tallies), jnp.arange(rows * top), side="right").astype(jnp.int32)
    listing = labels.reshape(top, rows).T
    listing = listing[jax.random.permutation(jax.random.fold_in(own, 1), rows)]
    offset_by = jax.random.randint(jax.random.fold_in(own, 2), (rows, 1), 0, top)
    return jnp.take_along_axis(listing, (jnp.arange(top)[None, :] + offset_by) % top, axis=1)


def load_shares(number_of, total, reach, lean, full):
    loads = [(1 << 20) // math.isqrt(rank ** lean) + 1 for rank in range(1, number_of + 1)]
    largest = reach if full else min(reach, max(-(-total // number_of), total * loads[0] // sum(loads)))
    least = 1 if total - largest >= number_of - 1 else 0
    given, rest = [largest] + [least] * (number_of - 1), total - largest - least * (number_of - 1)
    while rest > 0:
        candidates = [i for i in range(1, number_of) if given[i] < largest] or [i for i in range(1, number_of) if given[i] < reach]
        pool, budget = sum([loads[i] for i in candidates]), rest
        for i in candidates:
            more = min(reach - given[i], max(1, budget * loads[i] // pool), rest)
            given[i] = given[i] + more
            rest = rest - more
    return np.array(given)


def normal_values(key, dims, spread, limit, pieces=(), kind=jnp.bfloat16):
    values = jax.random.normal(key, dims, jnp.float32) * spread
    if len(pieces) > 0:
        values = steps_of(key, dims, pieces, -0.22, 0.18) * values
    return jnp.clip(values, min=-limit, max=limit).astype(kind)


def setup_inputs(seed: int = 0) -> dict:
    arg_keys = jax.random.split(jax.random.key(seed), 22)
    tokens = normal_values(arg_keys[0], (B, D), 1.0, 6.0, ((0, 16),))
    mix_gain = jnp.clip(1.0 + 0.18 * jax.random.normal(arg_keys[1], (D,), jnp.float32), 0.1, 1.9)
    w_query = normal_values(arg_keys[2], (D, HW), D ** -0.5, 0.125, ((0, 16), (1, 2)))
    w_key = normal_values(arg_keys[3], (D, HW), D ** -0.5, 0.125, ((0, 16), (1, 2)))
    w_value = normal_values(arg_keys[4], (D, HW), D ** -0.5, 0.125, ((0, 16), (1, 2)))
    w_outgate = normal_values(arg_keys[5], (D, HW), D ** -0.5, 0.125, ((0, 16), (1, 2)))
    w_igate = normal_values(arg_keys[6], (D, HEADS), D ** -0.5, 0.125, ((0, 16), (1, 2)))
    w_fgate = normal_values(arg_keys[7], (D, HEADS), D ** -0.5, 0.125, ((0, 16), (1, 2)))
    igate_bias = jnp.clip(-2.0 + 3.0 * jax.random.uniform(arg_keys[8], (HEADS,), jnp.float32) ** steps_of(arg_keys[8], (HEADS,), ((0, 2),), -0.2, 0.2), -2.0, 1.0)
    fgate_bias = jnp.clip(4.0 * jax.random.uniform(arg_keys[9], (HEADS,), jnp.float32) ** steps_of(arg_keys[9], (HEADS,), ((0, 2),), -0.2, 0.2), 0.0, 4.0)
    head_gain = jnp.clip(1.0 + 0.18 * jax.random.normal(arg_keys[10], (HW,), jnp.float32), 0.1, 1.9)
    w_out = normal_values(arg_keys[11], (HW, D), HW ** -0.5, 0.25, ((0, 2), (1, 16)))
    state_matrix = normal_values(arg_keys[12], (B, HEADS, HEAD_SIZE, HEAD_SIZE), 0.3, 2.4, ((0, 16), (1, 2)), jnp.float32)
    state_norm = normal_values(arg_keys[13], (B, HEADS, HEAD_SIZE), 0.3, 2.4, ((0, 16), (1, 2)), jnp.float32)
    state_max = normal_values(arg_keys[14], (B, HEADS), 1.0, 4.0, ((0, 16), (1, 2)), jnp.float32)
    ffn_gain = jnp.clip(1.0 + 0.18 * jax.random.normal(arg_keys[15], (D,), jnp.float32), 0.1, 1.9)
    w_expert_gate = normal_values(arg_keys[16], (EXPERTS, D, D_EXP), D ** -0.5, 0.125, ((0, 16), (2, 2)))
    w_expert_up = normal_values(arg_keys[17], (EXPERTS, D, D_EXP), D ** -0.5, 0.125, ((0, 16), (2, 2)))
    w_expert_down = normal_values(arg_keys[18], (EXPERTS, D_EXP, D), D_EXP ** -0.5, 0.15625, ((0, 16), (1, 2)))
    routes_keys = jax.random.split(jax.random.fold_in(arg_keys[19], 1), B // SEQ_DEV)
    routes_turns = jax.random.permutation(jax.random.fold_in(arg_keys[19], 3), B // SEQ_DEV)
    routes = jax.vmap(lambda own, number: routed_block(jax.random.fold_in(arg_keys[19], 2), own, number, SEQ_DEV, EXPERTS, TOPK, CAP, 2))(routes_keys, routes_turns).reshape((B, TOPK))
    route_weights = jnp.clip(0.2 + 0.8 * jax.random.uniform(arg_keys[20], (B, TOPK), jnp.float32) ** steps_of(arg_keys[20], (B, TOPK), ((0, 16),), -0.2, 0.2), 0.2, 1.0)
    return {"tokens": tokens, "mix_gain": mix_gain, "w_query": w_query, "w_key": w_key, "w_value": w_value, "w_outgate": w_outgate, "w_igate": w_igate, "w_fgate": w_fgate, "igate_bias": igate_bias, "fgate_bias": fgate_bias, "head_gain": head_gain, "w_out": w_out, "state_matrix": state_matrix, "state_norm": state_norm, "state_max": state_max, "ffn_gain": ffn_gain, "w_expert_gate": w_expert_gate, "w_expert_up": w_expert_up, "w_expert_down": w_expert_down, "routes": routes, "route_weights": route_weights}


def rms_scale(values_in, gain_vec):
    widened = values_in.astype(jnp.float32)
    return widened * lax.rsqrt(lax.optimization_barrier(jnp.mean(widened * widened, axis=-1, keepdims=True)) + 1e-06) * gain_vec

def memory_cell(query, key_row, value_row, outgate, input_pre, forget_pre, head_gain, state_matrix, state_norm, state_max):
    seq_rows, head_count = input_pre.shape
    head_size = query.shape[1] // head_count
    query_heads = query.astype(jnp.float32).reshape(seq_rows, head_count, head_size)
    key_heads = key_row.astype(jnp.float32).reshape(seq_rows, head_count, head_size) * head_size ** (-0.5)
    value_heads = value_row.astype(jnp.float32).reshape(seq_rows, head_count, head_size)
    log_forget = jax.nn.log_sigmoid(forget_pre)
    new_max = jnp.maximum(log_forget + state_max, input_pre)
    keep_old = jnp.exp(log_forget + state_max - new_max)
    keep_new = jnp.exp(input_pre - new_max)
    new_matrix = keep_old[:, :, None, None] * state_matrix + keep_new[:, :, None, None] * value_heads[:, :, :, None] * key_heads[:, :, None, :]
    new_norm = keep_old[:, :, None] * state_norm + keep_new[:, :, None] * key_heads
    numerator = jnp.einsum('bhvd,bhd->bhv', new_matrix, query_heads, precision=lax.Precision.HIGHEST)
    denominator = lax.optimization_barrier(jnp.sum(new_norm * query_heads, axis=-1))
    cell_read = numerator / jnp.maximum(jnp.abs(denominator), jnp.exp(-new_max))[:, :, None]
    centered = cell_read - lax.optimization_barrier(jnp.mean(cell_read, axis=-1, keepdims=True))
    variance = lax.optimization_barrier(jnp.mean(centered * centered, axis=-1, keepdims=True))
    scaled_cell = (centered * lax.rsqrt(variance + 1e-06)).reshape(seq_rows, head_count * head_size)
    cell_out = (scaled_cell * head_gain * jax.nn.sigmoid(outgate.astype(jnp.float32))).astype(jnp.bfloat16)
    return (cell_out, new_matrix, new_norm, new_max)

def reference(tokens, mix_gain, w_query, w_key, w_value, w_outgate, w_igate, w_fgate, igate_bias, fgate_bias, head_gain, w_out, state_matrix, state_norm, state_max, ffn_gain, w_expert_gate, w_expert_up, w_expert_down, routes, route_weights):
    normed = rms_scale(tokens, mix_gain).astype(jnp.bfloat16)

    def project(weight):
        return jnp.dot(normed, weight, preferred_element_type=jnp.float32)
    query = project(w_query).astype(jnp.bfloat16)
    key_row = project(w_key).astype(jnp.bfloat16)
    value_row = project(w_value).astype(jnp.bfloat16)
    outgate = project(w_outgate).astype(jnp.bfloat16)
    input_pre = project(w_igate) + igate_bias
    forget_pre = project(w_fgate) + fgate_bias
    cell_out, new_matrix, new_norm, new_max = memory_cell(query, key_row, value_row, outgate, input_pre, forget_pre, head_gain, state_matrix, state_norm, state_max)
    seq_rows, width = tokens.shape
    cell_width = cell_out.shape[1]
    blocks = jnp.einsum('bth,thd->btd', cell_out.astype(jnp.float32).reshape(seq_rows, N_TP, cell_width // N_TP), w_out.astype(jnp.float32).reshape(N_TP, cell_width // N_TP, width))
    rounded = lax.optimization_barrier(blocks.astype(jnp.bfloat16))
    resid = (tokens.astype(jnp.float32) + lax.optimization_barrier(jnp.sum(rounded.astype(jnp.float32), axis=1))).astype(jnp.bfloat16)
    normed_two = rms_scale(resid, ffn_gain).astype(jnp.bfloat16)
    groups = N_EP
    per_group = seq_rows // groups
    expert_total = w_expert_gate.shape[0]
    top_count = routes.shape[1]
    flat_routes = routes.reshape(groups, per_group * top_count)
    onehot = (flat_routes[:, :, None] == jnp.arange(expert_total, dtype=jnp.int32)[None, None, :]).astype(jnp.int32)
    earlier = jnp.cumsum(onehot, axis=1, dtype=jnp.int32) - onehot
    slots = lax.optimization_barrier(jnp.sum(onehot * earlier, axis=-1, dtype=jnp.int32)).astype(jnp.int32)
    group_ids = jnp.broadcast_to(jnp.arange(groups, dtype=jnp.int32)[:, None], flat_routes.shape)
    token_ids = (jnp.arange(seq_rows * top_count, dtype=jnp.int32) // top_count).reshape(groups, per_group * top_count)
    table = jnp.zeros((expert_total, groups, CAP), jnp.int32).at[flat_routes, group_ids, slots].set(token_ids)

    def run_expert(operands):
        gate_weight, up_weight, down_weight, row_ids = operands
        rows = normed_two[row_ids.reshape(-1)]
        gate_pre = jnp.dot(rows, gate_weight, preferred_element_type=jnp.float32)
        up_pre = jnp.dot(rows, up_weight, preferred_element_type=jnp.float32)
        hidden = (jax.nn.silu(gate_pre) * up_pre).astype(jnp.bfloat16)
        expert_width = hidden.shape[1]
        parts = jnp.einsum('rtf,tfd->rtd', hidden.astype(jnp.float32).reshape(-1, N_TP, expert_width // N_TP), down_weight.astype(jnp.float32).reshape(N_TP, expert_width // N_TP, width))
        rounded_parts = lax.optimization_barrier(parts.astype(jnp.bfloat16))
        return lax.optimization_barrier(jnp.sum(rounded_parts.astype(jnp.float32), axis=1)).astype(jnp.bfloat16)
    outputs = lax.map(run_expert, (w_expert_gate, w_expert_up, w_expert_down, table))
    picked = outputs[flat_routes, group_ids * CAP + slots]
    picked = picked.reshape(seq_rows, top_count, width).astype(jnp.float32)
    mixed = (resid.astype(jnp.float32) + lax.optimization_barrier(jnp.sum(picked * route_weights[:, :, None], axis=1))).astype(jnp.bfloat16)
    return (mixed, new_matrix, new_norm, new_max)
```

```python
import jax
import jax.numpy as jnp
from jax import lax
from jax.sharding import PartitionSpec as P


def rms_scale(values_in, gain_vec):
    widened = values_in.astype(jnp.float32)
    return (
        widened * lax.rsqrt(jnp.mean(widened * widened, axis=-1, keepdims=True) + 1e-06) * gain_vec
    )


def memory_cell(
    query,
    key_row,
    value_row,
    outgate,
    input_pre,
    forget_pre,
    head_gain,
    state_matrix,
    state_norm,
    state_max,
):
    seq_rows, head_count = input_pre.shape
    head_size = query.shape[1] // head_count
    query_heads = query.astype(jnp.float32).reshape(seq_rows, head_count, head_size)
    key_heads = key_row.astype(jnp.float32).reshape(
        seq_rows, head_count, head_size
    ) * head_size ** (-0.5)
    value_heads = value_row.astype(jnp.float32).reshape(seq_rows, head_count, head_size)
    log_forget = jax.nn.log_sigmoid(forget_pre)
    new_max = jnp.maximum(log_forget + state_max, input_pre)
    keep_old = jnp.exp(log_forget + state_max - new_max)
    keep_new = jnp.exp(input_pre - new_max)
    new_matrix = (
        keep_old[:, :, None, None] * state_matrix
        + keep_new[:, :, None, None] * value_heads[:, :, :, None] * key_heads[:, :, None, :]
    )
    new_norm = keep_old[:, :, None] * state_norm + keep_new[:, :, None] * key_heads
    numerator = jnp.einsum(
        "bhvd,bhd->bhv", new_matrix, query_heads, precision=lax.Precision.HIGHEST
    )
    denominator = jnp.sum(new_norm * query_heads, axis=-1)
    cell_read = numerator / jnp.maximum(jnp.abs(denominator), jnp.exp(-new_max))[:, :, None]
    centered = cell_read - jnp.mean(cell_read, axis=-1, keepdims=True)
    variance = jnp.mean(centered * centered, axis=-1, keepdims=True)
    scaled_cell = (centered * lax.rsqrt(variance + 1e-06)).reshape(seq_rows, head_count * head_size)
    cell_out = (scaled_cell * head_gain * jax.nn.sigmoid(outgate.astype(jnp.float32))).astype(
        jnp.bfloat16
    )
    return (cell_out, new_matrix, new_norm, new_max)


def torus_factors(count):
    side = 1
    while (2 * side) ** 3 <= count:
        side *= 2
    while count % (side * side):
        side -= 1
    return (count // (side * side), side, side)


def shift_pairs(factors, axis, step):
    pairs = []
    inner = 1
    for size in factors[axis + 1 :]:
        inner *= size
    total = factors[0] * factors[1] * factors[2]
    for source in range(total):
        place = source // inner % factors[axis]
        pairs.append((source, source + ((place + step) % factors[axis] - place) * inner))
    return pairs


def own_place(factors, axis):
    inner = 1
    for size in factors[axis + 1 :]:
        inner *= size
    return lax.axis_index("ep") // inner % factors[axis]


def reduce_stage(parts, factors, axis, dim):
    size = factors[axis]
    place = own_place(factors, axis)
    total = lax.dynamic_index_in_dim(parts, place, dim, keepdims=True).astype(jnp.float32)
    for step in range(1, size):
        sent = lax.dynamic_index_in_dim(parts, (place + step) % size, dim, keepdims=True)
        total = total + lax.ppermute(
            sent.astype(jnp.bfloat16), "ep", shift_pairs(factors, axis, step)
        ).astype(jnp.float32)
    return total


def staged_reduce_scatter(partial, factors, order):
    rows = partial.shape[0] // (factors[0] * factors[1] * factors[2])
    parts = partial.reshape(*factors, rows, partial.shape[1])
    for axis in order:
        parts = reduce_stage(parts, factors, axis, axis)
    return parts.reshape(rows, partial.shape[1])


def swap_cores(values_in):
    return lax.ppermute(values_in, "tp", [(0, 1), (1, 0)])


def body(
    tokens,
    mix_gain,
    w_query,
    w_key,
    w_value,
    w_outgate,
    w_igate,
    w_fgate,
    igate_bias,
    fgate_bias,
    head_gain,
    w_out,
    state_matrix,
    state_norm,
    state_max,
    ffn_gain,
    w_expert_gate,
    w_expert_up,
    w_expert_down,
    routes,
    route_weights,
):
    seq_rows, width = tokens.shape
    ep_count = lax.axis_size("ep")
    factors = torus_factors(ep_count)
    w_out_full = lax.all_gather(w_out, "ep", axis=1, tiled=True)

    local_experts = w_expert_gate.shape[0]
    expert_total = local_experts * ep_count
    top_count = routes.shape[1]
    capacity = max(2, 2 * seq_rows * top_count // expert_total)
    core_slots = -(-((capacity + 1) // 2) // 8) * 8
    core = lax.axis_index("tp")
    flat_routes = routes.reshape(-1)
    onehot = (flat_routes[:, None] == jnp.arange(expert_total, dtype=jnp.int32)[None, :]).astype(
        jnp.int32
    )
    earlier = jnp.cumsum(onehot, axis=0, dtype=jnp.int32) - onehot
    slots = jnp.sum(onehot * earlier, axis=1, dtype=jnp.int32)
    targets = jnp.where(slots % 2 == core, flat_routes * core_slots + slots // 2, -1)
    places = jnp.arange(expert_total * core_slots, dtype=jnp.int32)
    hits = (targets[:, None] == places[None, :]).reshape(seq_rows, top_count, -1)
    token_hits = jnp.any(hits, axis=1).astype(jnp.bfloat16)
    weight_hits = jnp.sum(jnp.where(hits, route_weights[:, :, None], 0.0), axis=1)

    normed = rms_scale(tokens, mix_gain).astype(jnp.bfloat16)
    spread = lax.all_to_all(normed, "ep", split_axis=1, concat_axis=0, tiled=True)
    first_list = (w_query, w_key)
    second_list = (w_value, w_outgate, w_igate, w_fgate)
    first = staged_reduce_scatter(
        jnp.dot(
            spread, jnp.concatenate(first_list, axis=1), preferred_element_type=jnp.float32
        ).astype(jnp.bfloat16),
        factors,
        (2, 1, 0),
    )
    second = staged_reduce_scatter(
        jnp.dot(
            spread, jnp.concatenate(second_list, axis=1), preferred_element_type=jnp.float32
        ).astype(jnp.bfloat16),
        factors,
        (1, 2, 0),
    )
    head_width = w_query.shape[1]
    head_count = w_igate.shape[1]
    query = first[:, :head_width].astype(jnp.bfloat16)
    key_row = first[:, head_width:].astype(jnp.bfloat16)
    value_row = second[:, :head_width].astype(jnp.bfloat16)
    outgate = second[:, head_width : 2 * head_width].astype(jnp.bfloat16)
    input_pre = second[:, 2 * head_width : 2 * head_width + head_count] + igate_bias
    forget_pre = second[:, 2 * head_width + head_count :] + fgate_bias
    cell_out, new_matrix, new_norm, new_max = memory_cell(
        query,
        key_row,
        value_row,
        outgate,
        input_pre,
        forget_pre,
        head_gain,
        state_matrix,
        state_norm,
        state_max,
    )
    partial_out = jnp.dot(cell_out, w_out_full, preferred_element_type=jnp.float32).astype(
        jnp.bfloat16
    )
    attended = partial_out.astype(jnp.float32) + swap_cores(partial_out).astype(jnp.float32)
    resid = (tokens.astype(jnp.float32) + attended).astype(jnp.bfloat16)
    normed_two = rms_scale(resid, ffn_gain).astype(jnp.bfloat16)

    outgoing = lax.dot_general(
        token_hits, normed_two, (((0,), (0,)), ((), ())), preferred_element_type=jnp.float32
    ).astype(jnp.bfloat16)
    outgoing = outgoing.reshape(expert_total, core_slots, width)
    received = lax.all_to_all(outgoing, "ep", split_axis=0, concat_axis=0, tiled=True)
    other = swap_cores(received)

    def grouped(rows):
        rows = rows.reshape(ep_count, local_experts, core_slots, width)
        return jnp.swapaxes(rows, 0, 1).reshape(local_experts, ep_count * core_slots, width)

    regrouped = jnp.concatenate([grouped(received), grouped(other)], axis=1)
    gate_pre = jnp.einsum("xcd,xdf->xcf", regrouped, w_expert_gate, preferred_element_type=jnp.float32)
    up_pre = jnp.einsum("xcd,xdf->xcf", regrouped, w_expert_up, preferred_element_type=jnp.float32)
    hidden = (jax.nn.silu(gate_pre) * up_pre).astype(jnp.bfloat16)
    partial_down = jnp.einsum(
        "xcf,xfd->xcd", hidden, w_expert_down, preferred_element_type=jnp.float32
    ).astype(jnp.bfloat16)
    half = ep_count * core_slots
    expert_sum = (
        partial_down[:, :half].astype(jnp.float32)
        + swap_cores(partial_down[:, half:]).astype(jnp.float32)
    ).astype(jnp.bfloat16)
    finished = jnp.swapaxes(
        expert_sum.reshape(local_experts, ep_count, core_slots, width), 0, 1
    ).reshape(ep_count * local_experts, core_slots, width)
    returned = lax.all_to_all(finished, "ep", split_axis=0, concat_axis=0, tiled=True)
    returned = returned.reshape(expert_total * core_slots, width)
    weight_high = weight_hits.astype(jnp.bfloat16)
    weight_rest = weight_hits - weight_high.astype(jnp.float32)
    weight_low = weight_rest.astype(jnp.bfloat16)
    weighted = jnp.dot(weight_high, returned, preferred_element_type=jnp.float32) + jnp.dot(
        weight_low, returned, preferred_element_type=jnp.float32
    )
    weighted = weighted + swap_cores(weighted)
    mixed = (resid.astype(jnp.float32) + weighted).astype(jnp.bfloat16)
    return (mixed, new_matrix, new_norm, new_max)


def solution(mesh):
    placed = (
        P("ep", None),
        P(),
        P("ep", "tp"),
        P("ep", "tp"),
        P("ep", "tp"),
        P("ep", "tp"),
        P("ep", "tp"),
        P("ep", "tp"),
        P("tp"),
        P("tp"),
        P("tp"),
        P("tp", "ep"),
        P("ep", "tp", None, None),
        P("ep", "tp", None),
        P("ep", "tp"),
        P(),
        P("ep", None, "tp"),
        P("ep", None, "tp"),
        P("ep", "tp", None),
        P("ep", None),
        P("ep", None),
    )
    return jax.shard_map(
        body,
        mesh=mesh,
        in_specs=placed,
        out_specs=(P("ep", None), P("ep", "tp", None, None), P("ep", "tp", None), P("ep", "tp")),
        check_vma=False,
    )
```

```python
import jax
import jax.numpy as jnp
from jax import lax
from jax.sharding import PartitionSpec as P


def rms_scale(values_in, gain_vec):
    widened = values_in.astype(jnp.float32)
    return (
        widened * lax.rsqrt(jnp.mean(widened * widened, axis=-1, keepdims=True) + 1e-06) * gain_vec
    )


def memory_cell(
    query,
    key_row,
    value_row,
    outgate,
    input_pre,
    forget_pre,
    head_gain,
    state_matrix,
    state_norm,
    state_max,
):
    seq_rows, head_count = input_pre.shape
    head_size = query.shape[1] // head_count
    query_heads = query.astype(jnp.float32).reshape(seq_rows, head_count, head_size)
    key_heads = key_row.astype(jnp.float32).reshape(
        seq_rows, head_count, head_size
    ) * head_size ** (-0.5)
    value_heads = value_row.astype(jnp.float32).reshape(seq_rows, head_count, head_size)
    log_forget = jax.nn.log_sigmoid(forget_pre)
    new_max = jnp.maximum(log_forget + state_max, input_pre)
    keep_old = jnp.exp(log_forget + state_max - new_max)
    keep_new = jnp.exp(input_pre - new_max)
    new_matrix = (
        keep_old[:, :, None, None] * state_matrix
        + keep_new[:, :, None, None] * value_heads[:, :, :, None] * key_heads[:, :, None, :]
    )
    new_norm = keep_old[:, :, None] * state_norm + keep_new[:, :, None] * key_heads
    numerator = jnp.sum(new_matrix * query_heads[:, :, None, :], axis=-1)
    denominator = jnp.sum(new_norm * query_heads, axis=-1)
    cell_read = numerator / jnp.maximum(jnp.abs(denominator), jnp.exp(-new_max))[:, :, None]
    centered = cell_read - jnp.mean(cell_read, axis=-1, keepdims=True)
    variance = jnp.mean(centered * centered, axis=-1, keepdims=True)
    scaled_cell = (centered * lax.rsqrt(variance + 1e-06)).reshape(seq_rows, head_count * head_size)
    cell_out = (scaled_cell * head_gain * jax.nn.sigmoid(outgate.astype(jnp.float32))).astype(
        jnp.bfloat16
    )
    return (cell_out, new_matrix, new_norm, new_max)


def torus_factors(count):
    side = 1
    while (2 * side) ** 3 <= count:
        side *= 2
    while count % (side * side):
        side -= 1
    return (count // (side * side), side, side)


def shift_pairs(factors, axis, step):
    pairs = []
    inner = 1
    for size in factors[axis + 1 :]:
        inner *= size
    total = factors[0] * factors[1] * factors[2]
    for source in range(total):
        place = source // inner % factors[axis]
        pairs.append((source, source + ((place + step) % factors[axis] - place) * inner))
    return pairs


def own_place(factors, axis):
    inner = 1
    for size in factors[axis + 1 :]:
        inner *= size
    return lax.axis_index("ep") // inner % factors[axis]


def reduce_stage(parts, factors, axis, dim):
    size = factors[axis]
    place = own_place(factors, axis)
    total = lax.dynamic_index_in_dim(parts, place, dim, keepdims=True).astype(jnp.float32)
    for step in range(1, size):
        sent = lax.dynamic_index_in_dim(parts, (place + step) % size, dim, keepdims=True)
        total = total + lax.ppermute(
            sent.astype(jnp.bfloat16), "ep", shift_pairs(factors, axis, step)
        ).astype(jnp.float32)
    return total


def staged_reduce_scatter(partial, factors, order):
    rows = partial.shape[0] // (factors[0] * factors[1] * factors[2])
    parts = partial.reshape(*factors, rows, partial.shape[1])
    for axis in order:
        parts = reduce_stage(parts, factors, axis, axis)
    return parts.reshape(rows, partial.shape[1])


def swap_cores(values_in):
    return lax.ppermute(values_in, "tp", [(0, 1), (1, 0)])


def body(
    tokens,
    mix_gain,
    w_query,
    w_key,
    w_value,
    w_outgate,
    w_igate,
    w_fgate,
    igate_bias,
    fgate_bias,
    head_gain,
    w_out,
    state_matrix,
    state_norm,
    state_max,
    ffn_gain,
    w_expert_gate,
    w_expert_up,
    w_expert_down,
    routes,
    route_weights,
):
    seq_rows, width = tokens.shape
    ep_count = lax.axis_size("ep")
    factors = torus_factors(ep_count)
    w_out_full = lax.all_gather(w_out, "ep", axis=1, tiled=True)

    local_experts = w_expert_gate.shape[0]
    expert_total = local_experts * ep_count
    top_count = routes.shape[1]
    capacity = max(2, 2 * seq_rows * top_count // expert_total)
    core_slots = -(-((capacity + 1) // 2) // 8) * 8
    core = lax.axis_index("tp")
    flat_routes = routes.reshape(-1)
    onehot = (flat_routes[:, None] == jnp.arange(expert_total, dtype=jnp.int32)[None, :]).astype(
        jnp.int32
    )
    earlier = jnp.cumsum(onehot, axis=0, dtype=jnp.int32) - onehot
    slots = jnp.sum(onehot * earlier, axis=1, dtype=jnp.int32)
    targets = jnp.where(slots % 2 == core, flat_routes * core_slots + slots // 2, -1)
    places = jnp.arange(expert_total * core_slots, dtype=jnp.int32)
    hits = (targets[:, None] == places[None, :]).reshape(seq_rows, top_count, -1)
    token_hits = jnp.any(hits, axis=1).astype(jnp.bfloat16)
    weight_hits = jnp.sum(jnp.where(hits, route_weights[:, :, None], 0.0), axis=1)

    normed = rms_scale(tokens, mix_gain).astype(jnp.bfloat16)
    spread = lax.all_to_all(normed, "ep", split_axis=1, concat_axis=0, tiled=True)
    first_list = (w_query, w_key)
    second_list = (w_value, w_outgate, w_igate, w_fgate)
    first = staged_reduce_scatter(
        jnp.dot(
            spread, jnp.concatenate(first_list, axis=1), preferred_element_type=jnp.float32
        ).astype(jnp.bfloat16),
        factors,
        (2, 1, 0),
    )
    second = staged_reduce_scatter(
        jnp.dot(
            spread, jnp.concatenate(second_list, axis=1), preferred_element_type=jnp.float32
        ).astype(jnp.bfloat16),
        factors,
        (1, 2, 0),
    )
    head_width = w_query.shape[1]
    head_count = w_igate.shape[1]
    query = first[:, :head_width].astype(jnp.bfloat16)
    key_row = first[:, head_width:].astype(jnp.bfloat16)
    value_row = second[:, :head_width].astype(jnp.bfloat16)
    outgate = second[:, head_width : 2 * head_width].astype(jnp.bfloat16)
    input_pre = second[:, 2 * head_width : 2 * head_width + head_count] + igate_bias
    forget_pre = second[:, 2 * head_width + head_count :] + fgate_bias
    cell_out, new_matrix, new_norm, new_max = memory_cell(
        query,
        key_row,
        value_row,
        outgate,
        input_pre,
        forget_pre,
        head_gain,
        state_matrix,
        state_norm,
        state_max,
    )
    partial_out = jnp.dot(cell_out, w_out_full, preferred_element_type=jnp.float32).astype(
        jnp.bfloat16
    )
    attended = partial_out.astype(jnp.float32) + swap_cores(partial_out).astype(jnp.float32)
    resid = (tokens.astype(jnp.float32) + attended).astype(jnp.bfloat16)
    normed_two = rms_scale(resid, ffn_gain).astype(jnp.bfloat16)

    outgoing = lax.dot_general(
        token_hits, normed_two, (((0,), (0,)), ((), ())), preferred_element_type=jnp.float32
    ).astype(jnp.bfloat16)
    outgoing = outgoing.reshape(expert_total, core_slots, width)
    received = lax.all_to_all(outgoing, "ep", split_axis=0, concat_axis=0, tiled=True)
    other = swap_cores(received)

    def grouped(rows):
        rows = rows.reshape(ep_count, local_experts, core_slots, width)
        return jnp.swapaxes(rows, 0, 1).reshape(local_experts, ep_count * core_slots, width)

    regrouped = jnp.concatenate([grouped(received), grouped(other)], axis=1)
    gate_pre = jnp.einsum("xcd,xdf->xcf", regrouped, w_expert_gate, preferred_element_type=jnp.float32)
    up_pre = jnp.einsum("xcd,xdf->xcf", regrouped, w_expert_up, preferred_element_type=jnp.float32)
    hidden = (jax.nn.silu(gate_pre) * up_pre).astype(jnp.bfloat16)
    partial_down = jnp.einsum(
        "xcf,xfd->xcd", hidden, w_expert_down, preferred_element_type=jnp.float32
    ).astype(jnp.bfloat16)
    half = ep_count * core_slots
    expert_sum = (
        partial_down[:, :half].astype(jnp.float32)
        + swap_cores(partial_down[:, half:]).astype(jnp.float32)
    ).astype(jnp.bfloat16)
    finished = jnp.swapaxes(
        expert_sum.reshape(local_experts, ep_count, core_slots, width), 0, 1
    ).reshape(ep_count * local_experts, core_slots, width)
    returned = lax.all_to_all(finished, "ep", split_axis=0, concat_axis=0, tiled=True)
    returned = returned.reshape(expert_total * core_slots, width)
    weight_high = weight_hits.astype(jnp.bfloat16)
    weight_rest = weight_hits - weight_high.astype(jnp.float32)
    weight_low = weight_rest.astype(jnp.bfloat16)
    weighted = jnp.dot(weight_high, returned, preferred_element_type=jnp.float32) + jnp.dot(
        weight_low, returned, preferred_element_type=jnp.float32
    )
    weighted = weighted + swap_cores(weighted)
    mixed = (resid.astype(jnp.float32) + weighted).astype(jnp.bfloat16)
    return (mixed, new_matrix, new_norm, new_max)


def solution(mesh):
    placed = (
        P("ep", None),
        P(),
        P("ep", "tp"),
        P("ep", "tp"),
        P("ep", "tp"),
        P("ep", "tp"),
        P("ep", "tp"),
        P("ep", "tp"),
        P("tp"),
        P("tp"),
        P("tp"),
        P("tp", "ep"),
        P("ep", "tp", None, None),
        P("ep", "tp", None),
        P("ep", "tp"),
        P(),
        P("ep", None, "tp"),
        P("ep", None, "tp"),
        P("ep", "tp", None),
        P("ep", None),
        P("ep", None),
    )
    return jax.shard_map(
        body,
        mesh=mesh,
        in_specs=placed,
        out_specs=(P("ep", None), P("ep", "tp", None, None), P("ep", "tp", None), P("ep", "tp")),
        check_vma=False,
    )
```
